32 devices in a mesh: sp: 8 (over z, x), tp: 4 (over y, core).
Axes of the slice: x: 2, y: 2, z: 4, core: 2. Of those that a mesh axis runs over, the one named last changes fastest.
Arguments:
- resid: bfloat16 [3072, 2048], P(('sp', 'tp')), may hold values from -6 to 6
- queries: bfloat16 [3072, 1024], P('sp', 'tp'), may hold values from -6 to 6
- keys: bfloat16 [3072, 1024], P('sp', 'tp'), may hold values from -6 to 6
- values: bfloat16 [3072, 1024], P('sp', 'tp'), may hold values from -6 to 6
- decay_input_part: bfloat16 [3072, 1024], P('sp', 'tp'), may hold values from -4 to 4
- decay_channel_offset: float32 [1024], P('tp'), may hold values from -16 to -2
- decay_head_extra: float32 [3072, 16], P('sp', 'tp'), may hold values from 0 to 0.7
- correction_rate_input: bfloat16 [3072, 1024], P('sp', 'tp'), may hold values from -6 to 6
- correction_rate_offset: float32 [1024], P('tp'), may hold values from -0.4 to 1
- head_norm_gain: float32 [1024], P('tp'), may hold values from 0.1 to 1.9
- mixer_output_weight: bfloat16 [1024, 2048], replicated, may hold values from -0.1875 to 0.1875
- feedforward_norm_gain: float32 [2048], replicated, may hold values from 0.1 to 1.9
- gate_weight: bfloat16 [2048, 5632], P('sp', 'tp'), may hold values from -0.125 to 0.125
- up_weight: bfloat16 [2048, 5632], P('sp', 'tp'), may hold values from -0.125 to 0.125
- down_weight: bfloat16 [5632, 2048], P('tp', 'sp'), may hold values from -0.078125 to 0.078125
Outputs:
- result: bfloat16 [3072, 2048], P(('sp', 'tp'))
The draws below stay inside these ranges and needn't reach their ends.
All inputs are finite; a program needn't handle non-finite values.
Results may differ from the reference program's by a relative error of at most 0.014.
Values may be sent and summed in bfloat16 or wider, within the bound.
A program may use at most 64 MiB of HBM per device.

```python
import math
import jax
import jax.numpy as jnp
from jax import lax

D = 2048
HEADS = 16
HEAD = 64
FF = 5632
TOK_DEV = 384
HW = 1024
TOKENS = 3072
N_SP = 8
N_TP = 4


def head_kinds(key, share):
    chosen = jax.random.uniform(jax.random.fold_in(key, 11), (HEADS,))
    return jnp.repeat(chosen < share, HEAD)


def draw_keys(key, part):
    flips = jax.random.bernoulli(jax.random.fold_in(key, 21), 0.5, (HEADS, HEAD))
    sizes = jax.random.uniform(jax.random.fold_in(key, 22), (HEADS, HEAD), jnp.float32, 0.5, 1.5)
    direction = jnp.where(flips, 1.0, -1.0) * sizes
    turns = jax.random.bernoulli(jax.random.fold_in(key, 23), 0.5, (TOKENS, HEADS))
    amounts = jax.random.uniform(jax.random.fold_in(key, 24), (TOKENS, HEADS), jnp.float32, 1.5, 3.0)
    amplitude = jnp.where(turns, 1.0, -1.0) * amounts
    spread = math.sqrt(6.0 * HEAD / TOKENS)
    noise = spread * jax.random.normal(jax.random.fold_in(key, 25), (TOKENS, HEADS, HEAD), jnp.float32)
    rows = amplitude[:, :, None] * direction[None] + noise
    return jnp.clip(rows, -6.0, 6.0).reshape(TOKENS, HEADS * HEAD).astype(jnp.bfloat16)


def draw_decay_channel_offset(key, part):
    share = 0.5
    slow = head_kinds(key, share)
    jitter = jax.random.uniform(jax.random.fold_in(key, 12), (HEADS * HEAD,), jnp.float32, -0.4, 0.4)
    quick = jax.random.uniform(jax.random.fold_in(key, 18), (HEADS * HEAD,), jnp.float32, -5.6, -2.4)
    return jnp.where(slow, math.log(0.3 / TOKENS) + 0.5 + jitter, quick)


def draw_correction_rate_offset(key, part):
    share = 0.5
    slow = head_kinds(key, share)
    jitter = jax.random.uniform(jax.random.fold_in(key, 13), (HEADS * HEAD,), jnp.float32, -0.4, 0.4)
    strong = jax.random.uniform(jax.random.fold_in(key, 19), (HEADS * HEAD,), jnp.float32, 0.2, 1.0)
    return jnp.where(slow, strong, jitter)


def draw_decay_head_extra(key, part):
    places = jax.random.randint(jax.random.fold_in(key, 14), (3, HEADS), 0, TOKENS)
    losses = jax.random.uniform(jax.random.fold_in(key, 15), (3, HEADS), jnp.float32, 0.22, 0.69)
    positions = jnp.arange(TOKENS, dtype=jnp.int32)[:, None, None]
    return jnp.sum(jnp.where(positions == places[None], losses[None], 0.0), axis=1)


def draw_decay_input_part(key, part):
    noise = 0.5 * jax.random.normal(jax.random.fold_in(key, 16), (TOKENS, HEADS * HEAD), jnp.float32)
    offset = jax.random.uniform(jax.random.fold_in(key, 17), (TOKENS // TOK_DEV, HEADS * HEAD), jnp.float32, -0.7, 0.7)
    return jnp.clip(noise + jnp.repeat(offset, TOK_DEV, axis=0), -4.0, 4.0).astype(jnp.bfloat16)


def steps_of(own_key, shape, split, low, top_value):
    factor_of = 1.0
    for dim, parts in split:
        draws = jax.random.uniform(jax.random.fold_in(jax.random.fold_in(own_key, 6), dim), (parts,), jnp.float32, low / len(split), top_value / len(split))
        factor_of = factor_of * jnp.repeat(jnp.exp(draws), shape[dim] // parts).reshape((-1,) + (1,) * (len(shape) - 1 - dim))
    return factor_of


def gaussian(rng, dims, deviation, reach, pieces=(), held_as=jnp.bfloat16):
    factor_of = steps_of(rng, dims, pieces, -0.22, 0.18) if pieces else 1.0
    array = jax.random.normal(rng, dims, jnp.float32) * deviation * factor_of
    return jnp.minimum(jnp.maximum(array, -reach), reach).astype(held_as)


def setup_inputs(seed: int = 0) -> dict:
    key_of = jax.random.split(jax.random.key(seed), 16)
    resid = gaussian(key_of[0], (TOKENS, D), 1.0, 6.0, ((0, 32),))
    queries = gaussian(key_of[1], (TOKENS, HW), 1.0, 6.0, ((0, 8), (1, 4)))
    keys = draw_keys(jax.random.fold_in(key_of[15], 71), 0)
    values = gaussian(key_of[3], (TOKENS, HW), 1.0, 6.0, ((0, 8), (1, 4)))
    decay_input_part = draw_decay_input_part(jax.random.fold_in(key_of[15], 71), 0)
    decay_channel_offset = draw_decay_channel_offset(jax.random.fold_in(key_of[15], 71), 0)
    decay_head_extra = draw_decay_head_extra(jax.random.fold_in(key_of[15], 71), 0)
    correction_rate_input = gaussian(key_of[7], (TOKENS, HW), 1.0, 6.0, ((0, 8), (1, 4)))
    correction_rate_offset = draw_correction_rate_offset(jax.random.fold_in(key_of[15], 71), 0)
    head_norm_gain = jnp.clip(1.0 + 0.18 * jax.random.normal(key_of[9], (HW,), jnp.float32), 0.1, 1.9)
    mixer_output_weight = gaussian(key_of[10], (HW, D), HW ** -0.5, 0.1875)
    feedforward_norm_gain = jnp.clip(1.0 + 0.18 * jax.random.normal(key_of[11], (D,), jnp.float32), 0.1, 1.9)
    gate_weight = gaussian(key_of[12], (D, FF), D ** -0.5, 0.125, ((0, 8), (1, 4)))
    up_weight = gaussian(key_of[13], (D, FF), D ** -0.5, 0.125, ((0, 8), (1, 4)))
    down_weight = gaussian(key_of[14], (FF, D), FF ** -0.5, 0.078125, ((0, 4), (1, 8)))
    return {"resid": resid, "queries": queries, "keys": keys, "values": values, "decay_input_part": decay_input_part, "decay_channel_offset": decay_channel_offset, "decay_head_extra": decay_head_extra, "correction_rate_input": correction_rate_input, "correction_rate_offset": correction_rate_offset, "head_norm_gain": head_norm_gain, "mixer_output_weight": mixer_output_weight, "feedforward_norm_gain": feedforward_norm_gain, "gate_weight": gate_weight, "up_weight": up_weight, "down_weight": down_weight}


def recurrence(carry_state, inputs):
    query_t, decay_t, key_t, value_t, unit_t, lrate_t = inputs
    lifted = jnp.einsum('hvk,hk->hv', carry_state, -unit_t, precision=lax.Precision.HIGHEST)
    carry_state = carry_state * decay_t[:, None, :] + lifted[:, :, None] * (unit_t * lrate_t)[:, None, :] + value_t[:, :, None] * key_t[:, None, :]
    return (carry_state, jnp.einsum('hvk,hk->hv', carry_state, query_t, precision=lax.Precision.HIGHEST))

def reference(resid, queries, keys, values, decay_input_part, decay_channel_offset, decay_head_extra, correction_rate_input, correction_rate_offset, head_norm_gain, mixer_output_weight, feedforward_norm_gain, gate_weight, up_weight, down_weight):

    def head_count(arr):
        return arr.astype(jnp.float32).reshape(TOKENS, HEADS, HEAD)
    correction_rate = jnp.exp(-jax.nn.softplus(-(decay_channel_offset + decay_input_part.astype(jnp.float32))) - 0.5)
    decay_factor = jnp.exp(-head_count(correction_rate) - decay_head_extra[:, :, None])
    key_f = head_count(keys)
    unit_keys = key_f * lax.rsqrt(lax.optimization_barrier(jnp.sum(key_f * key_f, axis=-1, keepdims=True)) + 1e-06)
    lrate = head_count(jax.nn.sigmoid(correction_rate_offset + correction_rate_input.astype(jnp.float32)))
    start = jnp.zeros((HEADS, HEAD, HEAD), jnp.float32)
    _, mixer_out = lax.scan(recurrence, start, (head_count(queries), decay_factor, key_f, head_count(values), unit_keys, lrate))
    center = mixer_out - lax.optimization_barrier(jnp.mean(mixer_out, axis=-1, keepdims=True))
    spread = lax.optimization_barrier(jnp.mean(center * center, axis=-1, keepdims=True))
    mixed = (center * lax.rsqrt(spread + 1e-05) * head_norm_gain.reshape(HEADS, HEAD)).reshape(TOKENS, HW).astype(jnp.bfloat16)

    def layer_block(pair):
        mixed_rows, resid_rows = pair
        proj = jnp.dot(mixed_rows, mixer_output_weight, preferred_element_type=jnp.float32)
        resid_mid = (resid_rows.astype(jnp.float32) + proj).astype(jnp.bfloat16)
        mid_f = resid_mid.astype(jnp.float32)
        normed = (mid_f * lax.rsqrt(lax.optimization_barrier(jnp.mean(mid_f * mid_f, axis=-1, keepdims=True)) + 1e-06) * feedforward_norm_gain).astype(jnp.bfloat16)
        gate = jnp.dot(normed, gate_weight, preferred_element_type=jnp.float32)
        upper = jnp.dot(normed, up_weight, preferred_element_type=jnp.float32)
        hidden = (jax.nn.silu(gate) * upper).astype(jnp.bfloat16)
        hid_parts = hidden.reshape(TOK_DEV, N_TP, FF // N_TP).astype(jnp.float32)
        down_parts = down_weight.reshape(N_TP, FF // N_TP, D).astype(jnp.float32)
        partial_value = jnp.einsum('tnf,nfd->ntd', hid_parts, down_parts).astype(jnp.bfloat16)
        partial_value = lax.optimization_barrier(partial_value).astype(jnp.float32)
        down_sum = lax.optimization_barrier(jnp.sum(partial_value, axis=0))
        return (mid_f + 0.5 * down_sum).astype(jnp.bfloat16)
    result = lax.map(layer_block, (mixed.reshape(N_SP, TOK_DEV, HW), resid.reshape(N_SP, TOK_DEV, D)))
    return result.reshape(TOKENS, D)
```

```python
import functools
import math

import jax
import jax.numpy as jnp
from jax import lax
from jax.experimental import pallas as pl
from jax.experimental.pallas import tpu as pltpu
from jax.sharding import Mesh, PartitionSpec as P

HEAD = 64
F32 = jnp.float32
BF16 = jnp.bfloat16


def split2(a):
    high = a.astype(BF16)
    return high, (a - high.astype(F32)).astype(BF16)


def dot3(a, b, dims):
    (ah, al), (bh, bl) = a, b
    dn = (dims, ((), ()))
    d = functools.partial(lax.dot_general, dimension_numbers=dn, preferred_element_type=F32)
    return d(ah, bh) + (d(ah, bl) + d(al, bh))


NN = ((1,), (0,))
NT = ((1,), (1,))
TN = ((0,), (0,))


def chunk_kernel(heads, chunk, q_ref, k_ref, v_ref, din_ref, doff_ref, extra_ref, rin_ref, roff_ref, reads_ref, total_ref, z_ref):
    rows = q_ref.shape[0]
    width = heads * HEAD
    wide = heads * chunk
    step = pl.program_id(0)

    @pl.when(step == 0)
    def _():
        r = lax.broadcasted_iota(jnp.int32, (width, 2 * HEAD), 0) % HEAD
        c = lax.broadcasted_iota(jnp.int32, (width, 2 * HEAD), 1)
        z_ref[...] = jnp.where(r == c, 1.0, 0.0).astype(F32)

    def load(ref):
        return ref[...].astype(F32)

    def stack(a):
        return jnp.concatenate([a[:, h * HEAD:(h + 1) * HEAD] for h in range(heads)], axis=0)

    spread_r = lax.broadcasted_iota(jnp.int32, (heads, width), 0)
    spread_c = lax.broadcasted_iota(jnp.int32, (heads, width), 1) // HEAD
    spread = jnp.where(spread_r == spread_c, 1.0, 0.0).astype(F32)
    extra = lax.dot_general(extra_ref[...], spread, ((((1,), (0,))), ((), ())), precision=lax.Precision.HIGHEST, preferred_element_type=F32)
    log_decay = -jax.nn.sigmoid(load(din_ref) + doff_ref[...]) * math.exp(-0.5) - extra
    tr = lax.broadcasted_iota(jnp.int32, (chunk, chunk), 0)
    tc = lax.broadcasted_iota(jnp.int32, (chunk, chunk), 1)
    lower = jnp.where(tr >= tc, 1.0, 0.0).astype(F32)
    cum = lax.dot_general(lower, log_decay, (((1,), (0,)), ((), ())), precision=lax.Precision.HIGHEST, preferred_element_type=F32)
    last = cum[chunk - 1:chunk, :]
    mid = cum[chunk // 2 - 1:chunk // 2, :]
    before = cum - log_decay
    rate = jax.nn.sigmoid(load(rin_ref) + roff_ref[...])

    key = stack(load(k_ref))
    unit = key * lax.rsqrt(jnp.sum(key * key, axis=-1, keepdims=True) + 1e-6)
    base = unit * stack(rate)
    query = stack(load(q_ref))
    value = split2(stack(load(v_ref)))
    to_mid = stack(jnp.exp(mid - cum))
    key_mid = split2(key * to_mid)
    base_mid = split2(base * to_mid)
    query_mid = split2(query * stack(jnp.exp(cum - mid)))
    unit_mid = split2(unit * stack(jnp.exp(before - mid)))
    to_last = stack(jnp.exp(last - cum))

    row = lax.broadcasted_iota(jnp.int32, (wide, wide), 0)
    col = lax.broadcasted_iota(jnp.int32, (wide, wide), 1)
    same = (row // chunk) == (col // chunk)
    strict = same & (row > col)
    upto = same & (row >= col)
    a_ub = jnp.where(strict, dot3(unit_mid, base_mid, NT), 0.0)
    a_uk = jnp.where(strict, dot3(unit_mid, key_mid, NT), 0.0)
    a_qb = jnp.where(upto, dot3(query_mid, base_mid, NT), 0.0)
    a_qk = jnp.where(upto, dot3(query_mid, key_mid, NT), 0.0)

    inverse = jnp.where(row == col, 1.0, 0.0).astype(F32)
    size = 1
    while size < chunk:
        pair = ((row // (2 * size)) == (col // (2 * size))) & ((row // size) > (col // size))
        part = jnp.where(pair, a_ub, 0.0)
        if size == 1:
            inverse = inverse - part
        else:
            inv = split2(inverse)
            inverse = inverse - dot3(split2(dot3(inv, split2(part), NN)), inv, NN)
        size *= 2
    inverse = split2(inverse)

    wr = lax.broadcasted_iota(jnp.int32, (wide, width), 0) // chunk
    wc = lax.broadcasted_iota(jnp.int32, (wide, width), 1) // HEAD

    def spread_wide(a):
        return jnp.where(wr == wc, jnp.concatenate([a] * heads, axis=1), 0.0)

    unit_wide = split2(spread_wide(unit * stack(jnp.exp(before))))
    query_wide = spread_wide(query * stack(jnp.exp(cum)))
    base_wide = split2(spread_wide(base * to_last))
    key_wide = split2(spread_wide(key * to_last))
    qb = split2(a_qb)
    trans = split2(dot3(inverse, unit_wide, NN))
    own = split2(dot3(inverse, split2(dot3(split2(a_uk), value, NN)), NN))
    read = split2(query_wide - dot3(qb, trans, NN))
    out_own = dot3(split2(a_qk), value, NN) - dot3(qb, own, NN)
    pr = lax.broadcasted_iota(jnp.int32, (width, width), 0)
    pc = lax.broadcasted_iota(jnp.int32, (width, width), 1)
    move = jnp.where(pr == pc, jnp.exp(last), 0.0) - dot3(base_wide, trans, TN)
    end = dot3(key_wide, value, TN) - dot3(base_wide, own, TN)

    z = split2(z_ref[...])
    x = dot3(read, z, NN) + jnp.concatenate([jnp.zeros_like(out_own), out_own], axis=1)
    for h in range(heads):
        reads_ref[h] = x[h * chunk:(h + 1) * chunk, :]
    z_new = dot3(split2(move), z, NN) + jnp.concatenate([jnp.zeros_like(end), end], axis=1)
    z_ref[...] = z_new
    total_ref[...] = z_new.astype(BF16)


def chunks(q, k, v, din, doff, extra, rin, roff):
    rows, width = q.shape
    heads = width // HEAD
    chunk = 64
    while rows % chunk:
        chunk //= 2
    tile = pl.BlockSpec((chunk, width), lambda i: (i, 0))
    vec = pl.BlockSpec((1, width), lambda i: (0, 0))
    n = rows // chunk
    return pl.pallas_call(
        functools.partial(chunk_kernel, heads, chunk),
        grid=(n,),
        in_specs=[tile, tile, tile, tile, vec, pl.BlockSpec((chunk, heads), lambda i: (i, 0)), tile, vec],
        out_specs=(
            pl.BlockSpec((heads, chunk, 2 * HEAD), lambda i: (0, i, 0)),
            pl.BlockSpec((width, 2 * HEAD), lambda i: (0, 0)),
        ),
        out_shape=(
            jax.ShapeDtypeStruct((heads, rows, 2 * HEAD), F32),
            jax.ShapeDtypeStruct((width, 2 * HEAD), BF16),
        ),
        scratch_shapes=[pltpu.VMEM((width, 2 * HEAD), F32)],
        compiler_params=pltpu.CompilerParams(dimension_semantics=("arbitrary",), vmem_limit_bytes=40 * 2**20),
    )(q, k, v, din, doff.reshape(1, width), extra, rin, roff.reshape(1, width))


def carry_kernel(nz, nx, total_ref, reads_ref, gain_ref, mixed_ref, held, send_sem, recv_sem):
    n = nz * nx
    me = lax.axis_index("z") * nx + lax.axis_index("x")
    heads = reads_ref.shape[0]

    def place(k):
        peer = lax.rem(me + k, n)
        return {"z": peer // nx, "x": lax.rem(peer, nx)}

    barrier = pltpu.get_barrier_semaphore()
    for k in range(1, n):
        pl.semaphore_signal(barrier, inc=1, device_id=place(k), device_id_type=pl.DeviceIdType.MESH)
    pl.semaphore_wait(barrier, n - 1)
    copies = []
    for k in range(1, n):
        c = pltpu.make_async_remote_copy(
            src_ref=total_ref, dst_ref=held.at[k], send_sem=send_sem.at[k], recv_sem=recv_sem.at[k],
            device_id=place(k), device_id_type=pl.DeviceIdType.MESH)
        c.start()
        copies.append(c)
    for c in copies:
        c.wait()
    state = [jnp.zeros((HEAD, HEAD), F32) for _ in range(heads)]
    for k in range(n - 1, 0, -1):
        there = k <= me
        for h in range(heads):
            block = held[k, h * HEAD:(h + 1) * HEAD, :].astype(F32)
            new = block[:, HEAD:] + jnp.dot(block[:, :HEAD], state[h], precision=lax.Precision.HIGHEST, preferred_element_type=F32)
            state[h] = jnp.where(there, new, state[h])
    outs = []
    for h in range(heads):
        x = reads_ref[h]
        o = x[:, HEAD:] + dot3(split2(x[:, :HEAD]), split2(state[h]), NN)
        center = o - jnp.mean(o, axis=-1, keepdims=True)
        var = jnp.mean(center * center, axis=-1, keepdims=True)
        outs.append(center * lax.rsqrt(var + 1e-5))
    mixed_ref[...] = (jnp.concatenate(outs, axis=1) * gain_ref[...]).astype(BF16)


def carry(total, reads, gain, nz, nx):
    heads, rows, _ = reads.shape
    width = heads * HEAD
    n = nz * nx
    vm = pl.BlockSpec(memory_space=pltpu.VMEM)
    return pl.pallas_call(
        functools.partial(carry_kernel, nz, nx),
        in_specs=[vm, vm, vm],
        out_specs=vm,
        out_shape=jax.ShapeDtypeStruct((rows, width), BF16),
        scratch_shapes=[
            pltpu.VMEM((n, width, 2 * HEAD), BF16),
            pltpu.SemaphoreType.DMA((n,)),
            pltpu.SemaphoreType.DMA((n,)),
        ],
        compiler_params=pltpu.CompilerParams(collective_id=1, has_side_effects=True, vmem_limit_bytes=24 * 2**20),
    )(total, reads, gain.reshape(1, width))


def send_z(block, nz):
    return [lax.ppermute(block, "z", [(s, (s + k) % nz) for s in range(nz)]) for k in range(1, nz)]


def in_order(block, came, nz, axis):
    z = lax.axis_index("z")
    size = block.shape[axis]
    shape = list(block.shape)
    shape[axis] = size * nz
    whole = jnp.zeros(shape, block.dtype)
    whole = lax.dynamic_update_slice_in_dim(whole, block, z * size, axis)
    for k in range(1, nz):
        whole = lax.dynamic_update_slice_in_dim(whole, came[k - 1], lax.rem(z - k + nz, nz) * size, axis)
    return whole


def per_device(
    nz, nx,
    resid, queries, keys, values, decay_input_part, decay_channel_offset, decay_head_extra,
    correction_rate_input, correction_rate_offset, head_norm_gain, mixer_output_weight,
    feedforward_norm_gain, gate_weight, up_weight, down_weight,
):
    ff = gate_weight.shape[1] // nx
    x = lax.axis_index("x")

    def exchange(weight, axis, join):
        pieces = weight.reshape(weight.shape[:axis] + (nx, ff) + weight.shape[axis + 1:])
        return lax.all_to_all(pieces, "x", split_axis=axis, concat_axis=join, tiled=False)

    def swap(weight, axis, join):
        if nx == 1:
            return weight
        if nx != 2:
            out = exchange(weight, axis, join)
            return out.reshape((-1, ff) if axis == 1 else (ff, -1))
        mine = lax.dynamic_slice_in_dim(weight, x * ff, ff, axis)
        other = lax.dynamic_slice_in_dim(weight, (1 - x) * ff, ff, axis)
        came = lax.ppermute(other, "x", [(0, 1), (1, 0)])
        first = jnp.where(x == 0, mine, came)
        second = jnp.where(x == 0, came, mine)
        return jnp.concatenate([first, second], axis=join)

    halves = (swap(gate_weight, 1, 0), swap(up_weight, 1, 0), swap(down_weight, 0, 1))
    halves, queries = lax.optimization_barrier((halves, queries))
    whole_gate = lax.all_gather(halves[0], "z", axis=0, tiled=True)
    up_came = send_z(halves[1], nz)
    down_came = send_z(halves[2], nz)

    reads, total = chunks(
        queries, keys, values, decay_input_part, decay_channel_offset, decay_head_extra,
        correction_rate_input, correction_rate_offset)
    total, up_came = lax.optimization_barrier((total, up_came))
    mixed = carry(total, reads, head_norm_gain, nz, nx)
    row_mixed = lax.all_to_all(mixed, "tp", split_axis=0, concat_axis=1, tiled=True)
    proj = jnp.dot(row_mixed, mixer_output_weight, preferred_element_type=F32)
    mid_f = (resid.astype(F32) + proj).astype(BF16).astype(F32)
    normed = (
        mid_f
        * lax.rsqrt(jnp.mean(mid_f * mid_f, axis=-1, keepdims=True) + 1e-06)
        * feedforward_norm_gain
    ).astype(BF16)
    normed, whole_gate = lax.optimization_barrier((normed, whole_gate))
    whole_up = in_order(halves[1], up_came, nz, 0)
    whole_down = in_order(halves[2], down_came, nz, 1)
    whole_rows = lax.all_gather(normed, ("x", "tp"), axis=0, tiled=True)
    gate = jnp.dot(whole_rows, whole_gate, preferred_element_type=F32)
    upper = jnp.dot(whole_rows, whole_up, preferred_element_type=F32)
    hidden = (jax.nn.silu(gate) * upper).astype(BF16)
    down_sum = lax.psum_scatter(
        jnp.dot(hidden, whole_down, preferred_element_type=F32).astype(BF16),
        ("x", "tp"), scatter_dimension=0, tiled=True,
    ).astype(F32)
    return (mid_f + 0.5 * down_sum).astype(BF16)


def solution(mesh):
    n_sp, n_tp = mesh.shape["sp"], mesh.shape["tp"]
    nx = 2 if n_sp % 2 == 0 else 1
    nz = n_sp // nx
    inner = Mesh(mesh.devices.reshape(nz, nx, n_tp), ("z", "x", "tp"))
    sp = ("z", "x")
    placed = (
        P(("z", "x", "tp"), None),
        P(sp, "tp"),
        P(sp, "tp"),
        P(sp, "tp"),
        P(sp, "tp"),
        P("tp"),
        P(sp, "tp"),
        P(sp, "tp"),
        P("tp"),
        P("tp"),
        P(),
        P(),
        P(sp, "tp"),
        P(sp, "tp"),
        P("tp", sp),
    )
    return jax.shard_map(
        functools.partial(per_device, nz, nx), mesh=inner, in_specs=placed,
        out_specs=P(("z", "x", "tp"), None), check_vma=False
    )
```
